32 devices in a mesh: grp: 2 (over y), sp: 4 (over z), dp: 4 (over x, core).
Axes of the slice: x: 2, y: 2, z: 4, core: 2. Of those that a mesh axis runs over, the one named last changes fastest.
Arguments:
- tokens: bfloat16 [8, 1536, 2048], P(('grp', 'dp'), 'sp'), parts along dimension 0, may hold values from -6 to 6
- w_value: bfloat16 [2048, 1024], P('dp', 'sp'), may hold values from -0.125 to 0.125
- w_gate: bfloat16 [2048, 1024], P('dp', 'sp'), may hold values from -0.125 to 0.125
- conv_weight: bfloat16 [31, 1024], replicated, may hold values from -20 to 20
- norm_gain: float32 [1024], replicated, may hold values from 0.1 to 1.9
- norm_bias: float32 [1024], replicated, may hold values from -3 to 3
- w_out: bfloat16 [1024, 2048], P('sp', 'dp'), may hold values from -0.1875 to 0.1875
Outputs:
- mixed: bfloat16 [8, 1536, 2048], P(('grp', 'dp'), 'sp'), parts along dimension 0
The draws below stay inside these ranges and needn't reach their ends.
There are 2 independent parts, one for each index of `grp`. The reference program is written for one: setup_inputs(seed, part) draws one part's arguments, and reference() takes and returns one part's arrays. A program takes and returns all parts, laid end to end along the dimension named above; an argument that names none is the same for every part. Nothing has to cross between parts.
All inputs are finite; a program needn't handle non-finite values.
Results may differ from the reference program's by a relative error of at most 0.012.
Values may be sent and summed in bfloat16 or wider, within the bound.
A program may use at most 64 MiB of HBM per device.

```python
import math
import jax
import jax.numpy as jnp
from jax import lax

D = 2048
C = 1024
KERNEL = 31
SEQ = 1536
SEQS = 4


def draw_conv_weight(key, part):
    first, second = jax.random.split(jax.random.fold_in(key, 11))
    ramp = jnp.arange(C, dtype=jnp.float32) / C
    base = jnp.clip(jax.random.normal(first, (KERNEL, C), jnp.float32), -4.0, 4.0)
    rising = jnp.exp(ramp * math.log(4.0))
    rough = jnp.exp(jax.random.uniform(second, (C,), jnp.float32, -0.7, 0.7))
    return (base * rising * rough / math.sqrt(KERNEL)).astype(jnp.bfloat16)


def block_levels(key, shape, shards, smallest, largest):
    loudness = 1.0
    for position, blocks in shards:
        heights = jax.random.uniform(jax.random.fold_in(jax.random.fold_in(key, 6), position), (blocks,), jnp.float32, smallest / len(shards), largest / len(shards))
        loudness = loudness * jnp.repeat(jnp.exp(heights), shape[position] // blocks).reshape((-1,) + (1,) * (len(shape) - 1 - position))
    return loudness


def bell_draw(rng, dims, scale, reach, cuts=(), kind=jnp.bfloat16):
    drawn = scale * jax.random.normal(rng, dims, jnp.float32)
    if cuts:
        drawn = drawn * block_levels(rng, dims, cuts, -0.22, 0.18)
    return jnp.clip(drawn, -reach, reach).astype(kind)


def setup_inputs(seed: int = 0, part: int = 0) -> dict:
    splits = jax.random.split(jax.random.key(seed), 8)
    part_splits = jax.random.split(jax.random.fold_in(splits[7], part), 8)
    return {
        "tokens": bell_draw(part_splits[0], (SEQS, SEQ, D), 1.0, 6.0, ((0, 4), (1, 4))),
        "w_value": bell_draw(splits[1], (D, C), D ** -0.5, 0.125, ((0, 4), (1, 4))),
        "w_gate": bell_draw(splits[2], (D, C), D ** -0.5, 0.125, ((0, 4), (1, 4))),
        "conv_weight": draw_conv_weight(jax.random.fold_in(splits[7], 71), part),
        "norm_gain": jnp.clip(1.0 + 0.18 * jax.random.normal(splits[4], (C,), jnp.float32), 0.1, 1.9),
        "norm_bias": bell_draw(splits[5], (C,), 0.5, 3.0, (), jnp.float32),
        "w_out": bell_draw(splits[6], (C, D), C ** -0.5, 0.1875, ((0, 4), (1, 4))),
    }


EPS = 1e-05

def one_sequence(seq_rows, w_value, w_gate, conv_weight, norm_gain, norm_bias, w_out):
    value = jnp.dot(seq_rows, w_value, preferred_element_type=jnp.float32)
    gate = jnp.dot(seq_rows, w_gate, preferred_element_type=jnp.float32)
    glu = (value * jax.nn.sigmoid(gate)).astype(jnp.bfloat16)
    length = glu.shape[0]
    glu_f = glu.astype(jnp.float32)
    padded = jnp.concatenate([jnp.zeros((KERNEL - 1, glu.shape[1]), jnp.float32), glu_f], axis=0)
    taps = conv_weight.astype(jnp.float32)
    total = jnp.zeros((length, glu.shape[1]), jnp.float32)
    for tap in range(KERNEL):
        begin = KERNEL - 1 - tap
        total = total + taps[tap][None, :] * padded[begin:begin + length]
    conv = total.astype(jnp.bfloat16)
    conv_f = conv.astype(jnp.float32)
    mean = lax.optimization_barrier(jnp.mean(conv_f, axis=1, keepdims=True))
    meansq = lax.optimization_barrier(jnp.mean(conv_f * conv_f, axis=1, keepdims=True))
    scaled = (conv_f - mean) * lax.rsqrt(meansq - mean * mean + EPS) * norm_gain + norm_bias
    normed = jax.nn.silu(scaled).astype(jnp.bfloat16)
    return jnp.dot(normed, w_out, preferred_element_type=jnp.float32).astype(jnp.bfloat16)

def reference(tokens, w_value, w_gate, conv_weight, norm_gain, norm_bias, w_out):
    return lax.map(lambda seq_rows: one_sequence(seq_rows, w_value, w_gate, conv_weight, norm_gain, norm_bias, w_out), tokens)
```

```python
import functools
import jax
import jax.numpy as jnp
from jax import lax
from jax.experimental import pallas as pl
from jax.experimental.pallas import tpu as pltpu
from jax.sharding import PartitionSpec as P

EPS = 1e-05
LANES = 128
PACK = 16
MESH = pl.DeviceIdType.MESH


def round_up(n, to):
    return -(-n // to) * to


def fused_kernel(
    n_sp,
    x_ref,
    wv_ref,
    wg_ref,
    wo_ref,
    cw_ref,
    gain_ref,
    bias_ref,
    out_ref,
    bv,
    bg,
    bo,
    xt,
    value,
    ext,
    taps,
    conv,
    normed,
    acc,
    stage,
    z_send,
    z_recv,
    x_send,
    x_recv,
    y_send,
    y_recv,
    c_send,
    c_recv,
    h_sem,
    l_sem,
    o_sem,
):
    z = lax.axis_index("sp")
    y = lax.axis_index("grp")
    dp = lax.axis_index("dp")
    core = lax.rem(dp, 2)
    twin = dp + 1 - 2 * core
    across = lax.rem(dp + 2, 4)
    n_dp = bo.shape[1]
    rows = x_ref.shape[0]
    total_rows = xt.shape[0]
    lead = total_rows - rows
    n_taps = cw_ref.shape[0]
    chunk = bv.shape[2]
    per_chunk = chunk // LANES
    groups = ext.shape[0]
    own = (wv_ref, wg_ref, wo_ref)
    bufs = (bv, bg, bo)

    def at_z(k):
        return lax.rem(z + k, n_sp)

    def span(m):
        size = own[m].shape[0]
        only = round_up(size * 5 // 16, PACK)
        return size, only, size - only

    def region(m, zz, dd, start, size):
        if m == 2:
            return bo.at[zz, dd, pl.ds(start, size), :]
        depth = own[m].shape[0]
        return bufs[m].at[zz, pl.ds(pl.multiple_of(dd * depth + start, PACK), size), :]

    def share(m):
        size, only, most = span(m)
        return pl.multiple_of(y * only, PACK), most

    def gives(m):
        size, only, most = span(m)
        return pl.multiple_of(y * most, PACK), only

    def lacks(m):
        size, only, most = span(m)
        return pl.multiple_of((1 - y) * most, PACK), only

    started = []

    def remote(src, dst, send, recv, where):
        return pltpu.make_async_remote_copy(
            src_ref=src, dst_ref=dst, send_sem=send, recv_sem=recv, device_id=where, device_id_type=MESH
        )

    def send(*a):
        copy = remote(*a)
        copy.start()
        started.append(copy)

    own_copies = [
        pltpu.make_async_copy(own[m], region(m, z, dp, 0, own[m].shape[0]), l_sem.at[m]) for m in range(3)
    ]
    x_copy = pltpu.make_async_copy(x_ref, xt.at[pl.ds(lead, rows), :], l_sem.at[3])
    for c in (own_copies[0], x_copy, own_copies[1], own_copies[2]):
        c.start()

    barrier = pltpu.get_barrier_semaphore()
    peers = [{"sp": at_z(k)} for k in range(1, n_sp)] + [{"dp": across}, {"grp": 1 - y}, {"dp": twin}]
    for peer in peers:
        pl.semaphore_signal(barrier, inc=1, device_id=peer, device_id_type=MESH)
    pl.semaphore_wait(barrier, len(peers))

    def own_share(m):
        start, size = share(m)
        return own[m].at[pl.ds(start, size), :], region(m, z, dp, start, size)

    def send_z(m, k):
        src, dst = own_share(m)
        send(src, dst, z_send.at[m, k - 1], z_recv.at[m, k - 1], {"sp": lax.rem(z + n_sp - k, n_sp)})

    def send_halo():
        send(
            x_ref.at[pl.ds(rows - lead, lead), :], xt.at[pl.ds(0, lead), :], h_sem.at[0], h_sem.at[1], {"sp": at_z(1)}
        )

    for m in range(3):
        src, dst = own_share(m)
        send_z(m, 1)
        send(src, dst, x_send.at[m, 0], x_recv.at[m, 0], {"dp": across})
        if m == 0:
            send_halo()
        for k in range(2, n_sp):
            send_z(m, k)
        whole = region(m, z, dp, 0, own[m].shape[0])
        send(own[m], whole, c_send.at[m, 0, 0], c_recv.at[m, 0, 0], {"dp": twin})

    for j in range(groups):
        taps[j, 0:n_taps, :] = cw_ref[:, j * LANES : (j + 1) * LANES].astype(jnp.float32)

    def forward_y(m, k, side, dd):
        start, size = gives(m)
        part = region(m, at_z(k), dd, start, size)
        send(part, part, y_send.at[m, k, side], y_recv.at[m, k, side], {"grp": 1 - y})

    def step_zx(m, k):
        start, size = share(m)
        if k > 0:
            part = region(m, at_z(k), dp, start, size)
            remote(part, part, z_send.at[m, k - 1], z_recv.at[m, k - 1], {"sp": z}).wait_recv()
            send(part, part, x_send.at[m, k], x_recv.at[m, k], {"dp": across})
            forward_y(m, k, 0, dp)
        part = region(m, at_z(k), across, start, size)
        remote(part, part, x_send.at[m, k], x_recv.at[m, k], {"dp": across}).wait_recv()
        forward_y(m, k, 1, across)

    def step_y(m, k):
        start, size = lacks(m)
        for side, dd in ((0, dp), (1, across)):
            if k == 0 and side == 0:
                continue
            part = region(m, at_z(k), dd, start, size)
            remote(part, part, y_send.at[m, k, side], y_recv.at[m, k, side], {"grp": 1 - y}).wait_recv()
            whole = region(m, at_z(k), dd, 0, own[m].shape[0])
            send(whole, whole, c_send.at[m, k, side], c_recv.at[m, k, side], {"dp": twin})

    def conv_group(j):
        tile = rows // 4
        for r in range(4):
            base = lead + r * tile
            total = jnp.zeros((tile, LANES), jnp.float32)
            for tap in range(n_taps):
                total = total + taps[j, tap : tap + 1, :] * ext[j, base - tap : base - tap + tile, :]
            conv[j, r * tile : (r + 1) * tile, :] = total.astype(jnp.bfloat16)

    def step_norm():
        tile = 2 * PACK
        channels = groups * LANES

        @pl.loop(0, rows // tile)
        def _(i):
            at = pl.ds(pl.multiple_of(i * tile, tile), tile)
            parts = [conv[j, at, :].astype(jnp.float32) for j in range(groups)]
            plain = functools.reduce(jnp.add, parts)
            square = functools.reduce(jnp.add, [p * p for p in parts])
            mean = jnp.sum(plain, axis=1, keepdims=True) * (1.0 / channels)
            meansq = jnp.sum(square, axis=1, keepdims=True) * (1.0 / channels)
            scale = lax.rsqrt(meansq - mean * mean + EPS)
            for j in range(groups):
                cols = slice(j * LANES, (j + 1) * LANES)
                v = (parts[j] - mean) * scale * gain_ref[:, cols] + bias_ref[:, cols]
                v = v / (1.0 + jnp.exp(-v))
                q, h = divmod(j, per_chunk)
                normed[q, at, h * LANES : (h + 1) * LANES] = v.astype(jnp.bfloat16)

    out_copies = []

    def step_use(m, k):
        zk = at_z(k)
        for side, dd in ((0, lax.rem(dp + 1 - 2 * core, n_dp)), (1, lax.rem(across + 1 - 2 * core, n_dp))):
            whole = region(m, zk, dd, 0, own[m].shape[0])
            remote(whole, whole, c_send.at[m, k, side], c_recv.at[m, k, side], {"dp": twin}).wait_recv()
        if k == 0:
            own_copies[m].wait()
            if m == 0:
                x_copy.wait()
                tail = xt.at[pl.ds(0, lead), :]
                remote(tail, tail, h_sem.at[0], h_sem.at[1], {"sp": z}).wait_recv()
        if m == 0:
            value[zk] = jnp.dot(xt[...], bv[zk], preferred_element_type=jnp.float32)
        elif m == 1:
            gate = jnp.dot(xt[...], bg[zk], preferred_element_type=jnp.float32)
            glu = (value[zk] * jax.nn.sigmoid(gate)).astype(jnp.bfloat16).astype(jnp.float32)
            before = jnp.where(z == 0, 0.0, 1.0)
            for h in range(per_chunk):
                cols = slice(h * LANES, (h + 1) * LANES)
                ext[zk * per_chunk + h, 0:lead, :] = glu[:lead, cols] * before
                ext[zk * per_chunk + h, lead:, :] = glu[lead:, cols]

            @pl.loop(0, per_chunk)
            def _(h):
                conv_group(zk * per_chunk + h)

            if k == n_sp - 1:
                step_norm()
        else:
            for d in range(n_dp):
                part = jnp.dot(normed[zk], bo[zk, d], preferred_element_type=jnp.float32)
                if k > 0:
                    part = part + acc[d]
                if k < n_sp - 1:
                    acc[d] = part
                else:
                    width = bo.shape[3]
                    stage[d] = part.astype(jnp.bfloat16)
                    copy = pltpu.make_async_copy(
                        stage.at[d], out_ref.at[:, d * width : (d + 1) * width], o_sem.at[d]
                    )
                    copy.start()
                    out_copies.append(copy)

    order = [(m, k) for m in range(3) for k in range(n_sp)]
    for t in range(len(order) + 2):
        if t < len(order):
            step_zx(*order[t])
        if 0 <= t - 1 < len(order):
            step_y(*order[t - 1])
        if t >= 2:
            step_use(*order[t - 2])

    for copy in started:
        copy.wait_send()
    for copy in out_copies:
        copy.wait()


def fused(n_sp, tokens, w_value, w_gate, conv_weight, norm_gain, norm_bias, w_out):
    rows, model = tokens.shape[1:]
    depth, chunk = w_value.shape
    deep, width = w_out.shape
    n_dp = model // depth
    n_taps, channels = conv_weight.shape
    lead = round_up(n_taps - 1, 2 * PACK)
    groups = channels // LANES
    total = rows + lead
    bf16, f32 = jnp.bfloat16, jnp.float32
    dma = pltpu.SemaphoreType.DMA
    anywhere = pl.BlockSpec(memory_space=pl.ANY)
    vmem = pl.BlockSpec(memory_space=pltpu.VMEM)
    out = pl.pallas_call(
        functools.partial(fused_kernel, n_sp),
        out_shape=jax.ShapeDtypeStruct((rows, model), bf16),
        in_specs=[anywhere] * 4 + [vmem] * 3,
        out_specs=anywhere,
        scratch_shapes=[
            pltpu.VMEM((n_sp, model, chunk), bf16),
            pltpu.VMEM((n_sp, model, chunk), bf16),
            pltpu.VMEM((n_sp, n_dp, deep, width), bf16),
            pltpu.VMEM((total, model), bf16),
            pltpu.VMEM((n_sp, total, chunk), f32),
            pltpu.VMEM((groups, total, LANES), f32),
            pltpu.VMEM((groups, round_up(n_taps, 8), LANES), f32),
            pltpu.VMEM((groups, rows, LANES), bf16),
            pltpu.VMEM((n_sp, rows, chunk), bf16),
            pltpu.VMEM((n_dp, rows, width), f32),
            pltpu.VMEM((n_dp, rows, width), bf16),
            dma((3, n_sp - 1)),
            dma((3, n_sp - 1)),
            dma((3, n_sp)),
            dma((3, n_sp)),
            dma((3, n_sp, 2)),
            dma((3, n_sp, 2)),
            dma((3, n_sp, 2)),
            dma((3, n_sp, 2)),
            dma((2,)),
            dma((4,)),
            dma((n_dp,)),
        ],
        compiler_params=pltpu.CompilerParams(
            collective_id=0, has_side_effects=True, vmem_limit_bytes=48 * 2**20
        ),
    )(tokens[0], w_value, w_gate, w_out, conv_weight, norm_gain[None], norm_bias[None])
    return out[None]


def passed_along(array, axis, by):
    peers = lax.axis_size(axis)
    pairs = [(i, i + by) for i in range(peers) if 0 <= i + by < peers]
    return lax.ppermute(array, axis, pairs)


def gathered(tokens, w_value, w_gate, conv_weight, norm_gain, norm_bias, w_out):
    pieces = (
        lax.all_gather(w_value, "sp", axis=1, tiled=True),
        lax.all_gather(w_gate, "sp", axis=1, tiled=True),
        lax.all_gather(w_out, "sp", axis=0, tiled=True),
    )
    full_value, full_gate, full_out = (
        lax.all_gather(pieces[0], "dp", axis=0, tiled=True),
        lax.all_gather(pieces[1], "dp", axis=0, tiled=True),
        lax.all_gather(pieces[2], "dp", axis=1, tiled=True),
    )
    rows = tokens[0]
    kernel_width = conv_weight.shape[0]
    channels = norm_gain.shape[0]
    value = jnp.dot(rows, full_value, preferred_element_type=jnp.float32)
    gate = jnp.dot(rows, full_gate, preferred_element_type=jnp.float32)
    glu = (value * jax.nn.sigmoid(gate)).astype(jnp.bfloat16)
    earlier = passed_along(glu[rows.shape[0] - (kernel_width - 1) :], "sp", 1)
    extended = jnp.concatenate([earlier, glu], axis=0)
    kernel = conv_weight[::-1][:, None, :]
    conv = lax.conv_general_dilated(
        extended[None],
        kernel,
        (1,),
        [(0, 0)],
        dimension_numbers=("NWC", "WIO", "NWC"),
        feature_group_count=channels,
        preferred_element_type=jnp.float32,
    )[0].astype(jnp.bfloat16)
    conv_f = conv.astype(jnp.float32)
    mean = jnp.mean(conv_f, axis=1, keepdims=True)
    meansq = jnp.mean(conv_f * conv_f, axis=1, keepdims=True)
    scaled = (conv_f - mean) * lax.rsqrt(meansq - mean * mean + EPS) * norm_gain + norm_bias
    normed = jax.nn.silu(scaled).astype(jnp.bfloat16)
    mixed = jnp.dot(normed, full_out, preferred_element_type=jnp.float32)
    return mixed.astype(jnp.bfloat16)[None]


def per_device(sizes, tokens, w_value, w_gate, conv_weight, norm_gain, norm_bias, w_out):
    args = (tokens, w_value, w_gate, conv_weight, norm_gain, norm_bias, w_out)
    pair_of_chips = sizes["grp"] == 2 and sizes["dp"] == 4
    whole_tiles = w_value.shape[1] % LANES == 0 and w_out.shape[1] % LANES == 0
    if pair_of_chips and whole_tiles and tokens.shape[0] == 1:
        return fused(sizes["sp"], *args)
    return gathered(*args)


def solution(mesh):
    placed = (
        P(("grp", "dp"), "sp", None),
        P("dp", "sp"),
        P("dp", "sp"),
        P(),
        P(),
        P(),
        P("sp", "dp"),
    )
    return jax.shard_map(
        functools.partial(per_device, dict(mesh.shape)),
        mesh=mesh,
        in_specs=placed,
        out_specs=P(("grp", "dp"), "sp", None),
        check_vma=False,
    )
```

```python
import functools
import jax
import jax.numpy as jnp
from jax import lax
from jax.experimental import pallas as pl
from jax.experimental.pallas import tpu as pltpu
from jax.sharding import PartitionSpec as P

EPS = 1e-05
LANES = 128
PACK = 16
MESH = pl.DeviceIdType.MESH


def round_up(n, to):
    return -(-n // to) * to


def fused_kernel(
    n_sp,
    x_ref,
    wv_ref,
    wg_ref,
    wo_ref,
    cw_ref,
    gain_ref,
    bias_ref,
    out_ref,
    bv,
    bg,
    bo,
    xt,
    value,
    ext,
    taps,
    conv,
    normed,
    acc,
    stage,
    z_send,
    z_recv,
    x_send,
    x_recv,
    y_send,
    y_recv,
    c_send,
    c_recv,
    h_sem,
    l_sem,
    o_sem,
):
    z = lax.axis_index("sp")
    y = lax.axis_index("grp")
    dp = lax.axis_index("dp")
    core = lax.rem(dp, 2)
    twin = dp + 1 - 2 * core
    across = lax.rem(dp + 2, 4)
    n_dp = bo.shape[1]
    rows = x_ref.shape[0]
    total_rows = xt.shape[0]
    lead = total_rows - rows
    n_taps = cw_ref.shape[0]
    chunk = bv.shape[2]
    per_chunk = chunk // LANES
    groups = ext.shape[0]
    own = (wv_ref, wg_ref, wo_ref)
    bufs = (bv, bg, bo)

    def at_z(k):
        return lax.rem(z + k, n_sp)

    def span(m):
        size = own[m].shape[0]
        only = round_up(size * 5 // 16, PACK)
        return size, only, size - only

    def region(m, zz, dd, start, size):
        if m == 2:
            return bo.at[zz, dd, pl.ds(start, size), :]
        depth = own[m].shape[0]
        return bufs[m].at[zz, pl.ds(pl.multiple_of(dd * depth + start, PACK), size), :]

    def share(m):
        size, only, most = span(m)
        return pl.multiple_of(y * only, PACK), most

    def gives(m):
        size, only, most = span(m)
        return pl.multiple_of(y * most, PACK), only

    def lacks(m):
        size, only, most = span(m)
        return pl.multiple_of((1 - y) * most, PACK), only

    started = []

    def remote(src, dst, send, recv, where):
        return pltpu.make_async_remote_copy(
            src_ref=src, dst_ref=dst, send_sem=send, recv_sem=recv, device_id=where, device_id_type=MESH
        )

    def send(*a):
        copy = remote(*a)
        copy.start()
        started.append(copy)

    own_copies = [
        pltpu.make_async_copy(own[m], region(m, z, dp, 0, own[m].shape[0]), l_sem.at[m]) for m in range(3)
    ]
    x_copy = pltpu.make_async_copy(x_ref, xt.at[pl.ds(lead, rows), :], l_sem.at[3])
    for c in (own_copies[0], x_copy, own_copies[1], own_copies[2]):
        c.start()

    barrier = pltpu.get_barrier_semaphore()
    peers = [{"sp": at_z(k)} for k in range(1, n_sp)] + [{"dp": across}, {"grp": 1 - y}, {"dp": twin}]
    for peer in peers:
        pl.semaphore_signal(barrier, inc=1, device_id=peer, device_id_type=MESH)
    pl.semaphore_wait(barrier, len(peers))

    def own_share(m):
        start, size = share(m)
        return own[m].at[pl.ds(start, size), :], region(m, z, dp, start, size)

    def send_z(m, k):
        src, dst = own_share(m)
        send(src, dst, z_send.at[m, k - 1], z_recv.at[m, k - 1], {"sp": lax.rem(z + n_sp - k, n_sp)})

    def send_halo():
        send(
            x_ref.at[pl.ds(rows - lead, lead), :], xt.at[pl.ds(0, lead), :], h_sem.at[0], h_sem.at[1], {"sp": at_z(1)}
        )

    for m in range(3):
        src, dst = own_share(m)
        send_z(m, 1)
        send(src, dst, x_send.at[m, 0], x_recv.at[m, 0], {"dp": across})
        if m == 0:
            send_halo()
        for k in range(2, n_sp):
            send_z(m, k)
        whole = region(m, z, dp, 0, own[m].shape[0])
        send(own[m], whole, c_send.at[m, 0, 0], c_recv.at[m, 0, 0], {"dp": twin})

    for j in range(groups):
        taps[j, 0:n_taps, :] = cw_ref[:, j * LANES : (j + 1) * LANES].astype(jnp.float32)

    def forward_y(m, k, side, dd):
        start, size = gives(m)
        part = region(m, at_z(k), dd, start, size)
        send(part, part, y_send.at[m, k, side], y_recv.at[m, k, side], {"grp": 1 - y})

    def step_z(m, k):
        start, size = share(m)
        if k > 0:
            part = region(m, at_z(k), dp, start, size)
            remote(part, part, z_send.at[m, k - 1], z_recv.at[m, k - 1], {"sp": z}).wait_recv()
            send(part, part, x_send.at[m, k], x_recv.at[m, k], {"dp": across})
            forward_y(m, k, 0, dp)

    def step_x(m, k):
        start, size = share(m)
        part = region(m, at_z(k), across, start, size)
        remote(part, part, x_send.at[m, k], x_recv.at[m, k], {"dp": across}).wait_recv()
        forward_y(m, k, 1, across)

    def step_y(m, k):
        start, size = lacks(m)
        for side, dd in ((0, dp), (1, across)):
            if k == 0 and side == 0:
                continue
            part = region(m, at_z(k), dd, start, size)
            remote(part, part, y_send.at[m, k, side], y_recv.at[m, k, side], {"grp": 1 - y}).wait_recv()
            whole = region(m, at_z(k), dd, 0, own[m].shape[0])
            send(whole, whole, c_send.at[m, k, side], c_recv.at[m, k, side], {"dp": twin})

    def conv_group(j):
        tile = rows // 4
        for r in range(4):
            base = lead + r * tile
            total = jnp.zeros((tile, LANES), jnp.float32)
            for tap in range(n_taps):
                total = total + taps[j, tap : tap + 1, :] * ext[j, base - tap : base - tap + tile, :]
            conv[j, r * tile : (r + 1) * tile, :] = total.astype(jnp.bfloat16)

    def step_norm():
        tile = 2 * PACK
        channels = groups * LANES

        @pl.loop(0, rows // tile)
        def _(i):
            at = pl.ds(pl.multiple_of(i * tile, tile), tile)
            parts = [conv[j, at, :].astype(jnp.float32) for j in range(groups)]
            plain = functools.reduce(jnp.add, parts)
            square = functools.reduce(jnp.add, [p * p for p in parts])
            mean = jnp.sum(plain, axis=1, keepdims=True) * (1.0 / channels)
            meansq = jnp.sum(square, axis=1, keepdims=True) * (1.0 / channels)
            scale = lax.rsqrt(meansq - mean * mean + EPS)
            for j in range(groups):
                cols = slice(j * LANES, (j + 1) * LANES)
                v = (parts[j] - mean) * scale * gain_ref[:, cols] + bias_ref[:, cols]
                v = v / (1.0 + jnp.exp(-v))
                q, h = divmod(j, per_chunk)
                normed[q, at, h * LANES : (h + 1) * LANES] = v.astype(jnp.bfloat16)

    out_copies = []

    def step_use(m, k):
        zk = at_z(k)
        for side, dd in ((0, lax.rem(dp + 1 - 2 * core, n_dp)), (1, lax.rem(across + 1 - 2 * core, n_dp))):
            whole = region(m, zk, dd, 0, own[m].shape[0])
            remote(whole, whole, c_send.at[m, k, side], c_recv.at[m, k, side], {"dp": twin}).wait_recv()
        if k == 0:
            own_copies[m].wait()
            if m == 0:
                x_copy.wait()
                tail = xt.at[pl.ds(0, lead), :]
                remote(tail, tail, h_sem.at[0], h_sem.at[1], {"sp": z}).wait_recv()
        if m == 0:
            value[zk] = jnp.dot(xt[...], bv[zk], preferred_element_type=jnp.float32)
        elif m == 1:
            gate = jnp.dot(xt[...], bg[zk], preferred_element_type=jnp.float32)
            glu = (value[zk] * jax.nn.sigmoid(gate)).astype(jnp.bfloat16).astype(jnp.float32)
            before = jnp.where(z == 0, 0.0, 1.0)
            for h in range(per_chunk):
                cols = slice(h * LANES, (h + 1) * LANES)
                ext[zk * per_chunk + h, 0:lead, :] = glu[:lead, cols] * before
                ext[zk * per_chunk + h, lead:, :] = glu[lead:, cols]

            @pl.loop(0, per_chunk)
            def _(h):
                conv_group(zk * per_chunk + h)

            if k == n_sp - 1:
                step_norm()
        else:
            for d in range(n_dp):
                part = jnp.dot(normed[zk], bo[zk, d], preferred_element_type=jnp.float32)
                if k > 0:
                    part = part + acc[d]
                if k < n_sp - 1:
                    acc[d] = part
                else:
                    width = bo.shape[3]
                    stage[d] = part.astype(jnp.bfloat16)
                    copy = pltpu.make_async_copy(
                        stage.at[d], out_ref.at[:, d * width : (d + 1) * width], o_sem.at[d]
                    )
                    copy.start()
                    out_copies.append(copy)

    order = [(m, k) for m in range(3) for k in range(n_sp)]
    lags = ((step_z, 0), (step_x, 2), (step_y, 4), (step_use, 5))
    for t in range(len(order) + lags[-1][1]):
        for step, lag in lags:
            if 0 <= t - lag < len(order):
                step(*order[t - lag])

    for copy in started:
        copy.wait_send()
    for copy in out_copies:
        copy.wait()


def fused(n_sp, tokens, w_value, w_gate, conv_weight, norm_gain, norm_bias, w_out):
    rows, model = tokens.shape[1:]
    depth, chunk = w_value.shape
    deep, width = w_out.shape
    n_dp = model // depth
    n_taps, channels = conv_weight.shape
    lead = round_up(n_taps - 1, 2 * PACK)
    groups = channels // LANES
    total = rows + lead
    bf16, f32 = jnp.bfloat16, jnp.float32
    dma = pltpu.SemaphoreType.DMA
    anywhere = pl.BlockSpec(memory_space=pltpu.HBM)
    vmem = pl.BlockSpec(memory_space=pltpu.VMEM)
    out = pl.pallas_call(
        functools.partial(fused_kernel, n_sp),
        out_shape=jax.ShapeDtypeStruct((rows, model), bf16),
        in_specs=[anywhere] * 4 + [vmem] * 3,
        out_specs=anywhere,
        scratch_shapes=[
            pltpu.VMEM((n_sp, model, chunk), bf16),
            pltpu.VMEM((n_sp, model, chunk), bf16),
            pltpu.VMEM((n_sp, n_dp, deep, width), bf16),
            pltpu.VMEM((total, model), bf16),
            pltpu.VMEM((n_sp, total, chunk), f32),
            pltpu.VMEM((groups, total, LANES), f32),
            pltpu.VMEM((groups, round_up(n_taps, 8), LANES), f32),
            pltpu.VMEM((groups, rows, LANES), bf16),
            pltpu.VMEM((n_sp, rows, chunk), bf16),
            pltpu.VMEM((n_dp, rows, width), f32),
            pltpu.VMEM((n_dp, rows, width), bf16),
            dma((3, n_sp - 1)),
            dma((3, n_sp - 1)),
            dma((3, n_sp)),
            dma((3, n_sp)),
            dma((3, n_sp, 2)),
            dma((3, n_sp, 2)),
            dma((3, n_sp, 2)),
            dma((3, n_sp, 2)),
            dma((2,)),
            dma((4,)),
            dma((n_dp,)),
        ],
        compiler_params=pltpu.CompilerParams(
            collective_id=0, has_side_effects=True, vmem_limit_bytes=63 * 2**20
        ),
    )(tokens[0], w_value, w_gate, w_out, conv_weight, norm_gain[None], norm_bias[None])
    return out[None]


def passed_along(array, axis, by):
    peers = lax.axis_size(axis)
    pairs = [(i, i + by) for i in range(peers) if 0 <= i + by < peers]
    return lax.ppermute(array, axis, pairs)


def gathered(tokens, w_value, w_gate, conv_weight, norm_gain, norm_bias, w_out):
    pieces = (
        lax.all_gather(w_value, "sp", axis=1, tiled=True),
        lax.all_gather(w_gate, "sp", axis=1, tiled=True),
        lax.all_gather(w_out, "sp", axis=0, tiled=True),
    )
    full_value, full_gate, full_out = (
        lax.all_gather(pieces[0], "dp", axis=0, tiled=True),
        lax.all_gather(pieces[1], "dp", axis=0, tiled=True),
        lax.all_gather(pieces[2], "dp", axis=1, tiled=True),
    )
    rows = tokens[0]
    kernel_width = conv_weight.shape[0]
    channels = norm_gain.shape[0]
    value = jnp.dot(rows, full_value, preferred_element_type=jnp.float32)
    gate = jnp.dot(rows, full_gate, preferred_element_type=jnp.float32)
    glu = (value * jax.nn.sigmoid(gate)).astype(jnp.bfloat16)
    earlier = passed_along(glu[rows.shape[0] - (kernel_width - 1) :], "sp", 1)
    extended = jnp.concatenate([earlier, glu], axis=0)
    kernel = conv_weight[::-1][:, None, :]
    conv = lax.conv_general_dilated(
        extended[None],
        kernel,
        (1,),
        [(0, 0)],
        dimension_numbers=("NWC", "WIO", "NWC"),
        feature_group_count=channels,
        preferred_element_type=jnp.float32,
    )[0].astype(jnp.bfloat16)
    conv_f = conv.astype(jnp.float32)
    mean = jnp.mean(conv_f, axis=1, keepdims=True)
    meansq = jnp.mean(conv_f * conv_f, axis=1, keepdims=True)
    scaled = (conv_f - mean) * lax.rsqrt(meansq - mean * mean + EPS) * norm_gain + norm_bias
    normed = jax.nn.silu(scaled).astype(jnp.bfloat16)
    mixed = jnp.dot(normed, full_out, preferred_element_type=jnp.float32)
    return mixed.astype(jnp.bfloat16)[None]


def per_device(sizes, tokens, w_value, w_gate, conv_weight, norm_gain, norm_bias, w_out):
    args = (tokens, w_value, w_gate, conv_weight, norm_gain, norm_bias, w_out)
    pair_of_chips = sizes["grp"] == 2 and sizes["dp"] == 4
    whole_tiles = w_value.shape[1] % LANES == 0 and w_out.shape[1] % LANES == 0
    if pair_of_chips and whole_tiles and tokens.shape[0] == 1:
        return fused(sizes["sp"], *args)
    return gathered(*args)


def solution(mesh):
    placed = (
        P(("grp", "dp"), "sp", None),
        P("dp", "sp"),
        P("dp", "sp"),
        P(),
        P(),
        P(),
        P("sp", "dp"),
    )
    return jax.shard_map(
        functools.partial(per_device, dict(mesh.shape)),
        mesh=mesh,
        in_specs=placed,
        out_specs=P(("grp", "dp"), "sp", None),
        check_vma=False,
    )
```

```python
import functools
import jax
import jax.numpy as jnp
from jax import lax
from jax.experimental import pallas as pl
from jax.experimental.pallas import tpu as pltpu
from jax.sharding import PartitionSpec as P

EPS = 1e-05
LANES = 128
PACK = 16
MESH = pl.DeviceIdType.MESH


def round_up(n, to):
    return -(-n // to) * to


def fused_kernel(
    n_sp,
    x_ref,
    wv_ref,
    wg_ref,
    wo_ref,
    cw_ref,
    gain_ref,
    bias_ref,
    out_ref,
    bv,
    bg,
    bo,
    xt,
    value,
    ext,
    taps,
    conv,
    normed,
    acc,
    stage,
    z_send,
    z_recv,
    x_send,
    x_recv,
    y_send,
    y_recv,
    c_send,
    c_recv,
    h_sem,
    l_sem,
    o_sem,
):
    z = lax.axis_index("sp")
    y = lax.axis_index("grp")
    dp = lax.axis_index("dp")
    core = lax.rem(dp, 2)
    twin = dp + 1 - 2 * core
    across = lax.rem(dp + 2, 4)
    n_dp = bo.shape[1]
    rows = x_ref.shape[0]
    total_rows = xt.shape[0]
    lead = total_rows - rows
    n_taps = cw_ref.shape[0]
    chunk = bv.shape[2]
    per_chunk = chunk // LANES
    groups = ext.shape[0]
    own = (wv_ref, wg_ref, wo_ref)
    bufs = (bv, bg, bo)

    def at_z(k):
        return lax.rem(z + k, n_sp)

    def span(m):
        size = own[m].shape[0]
        only = round_up(size * (4 if m == 2 else 6) // 16, PACK)
        return size, only, size - only

    def region(m, zz, dd, start, size):
        if m == 2:
            return bo.at[zz, dd, pl.ds(start, size), :]
        depth = own[m].shape[0]
        return bufs[m].at[zz, pl.ds(pl.multiple_of(dd * depth + start, PACK), size), :]

    def share(m):
        size, only, most = span(m)
        return pl.multiple_of(y * only, PACK), most

    def gives(m):
        size, only, most = span(m)
        return pl.multiple_of(y * most, PACK), only

    def lacks(m):
        size, only, most = span(m)
        return pl.multiple_of((1 - y) * most, PACK), only

    started = []

    def remote(src, dst, send, recv, where):
        return pltpu.make_async_remote_copy(
            src_ref=src, dst_ref=dst, send_sem=send, recv_sem=recv, device_id=where, device_id_type=MESH
        )

    def send(*a):
        copy = remote(*a)
        copy.start()
        started.append(copy)

    own_copies = [
        pltpu.make_async_copy(own[m], region(m, z, dp, 0, own[m].shape[0]), l_sem.at[m]) for m in range(3)
    ]
    x_copy = pltpu.make_async_copy(x_ref, xt.at[pl.ds(lead, rows), :], l_sem.at[3])
    for c in (own_copies[0], x_copy, own_copies[1], own_copies[2]):
        c.start()

    barrier = pltpu.get_barrier_semaphore()
    peers = [{"sp": at_z(k)} for k in range(1, n_sp)] + [{"dp": across}, {"grp": 1 - y}, {"dp": twin}]
    for peer in peers:
        pl.semaphore_signal(barrier, inc=1, device_id=peer, device_id_type=MESH)
    pl.semaphore_wait(barrier, len(peers))

    def own_share(m):
        start, size = share(m)
        return own[m].at[pl.ds(start, size), :], region(m, z, dp, start, size)

    def send_z(m, k):
        src, dst = own_share(m)
        send(src, dst, z_send.at[m, k - 1], z_recv.at[m, k - 1], {"sp": lax.rem(z + n_sp - k, n_sp)})

    def send_halo():
        send(
            x_ref.at[pl.ds(rows - lead, lead), :], xt.at[pl.ds(0, lead), :], h_sem.at[0], h_sem.at[1], {"sp": at_z(1)}
        )

    for m in range(3):
        src, dst = own_share(m)
        send_z(m, 1)
        send(src, dst, x_send.at[m, 0], x_recv.at[m, 0], {"dp": across})
        if m == 0:
            send_halo()
        for k in range(2, n_sp):
            send_z(m, k)
        whole = region(m, z, dp, 0, own[m].shape[0])
        send(own[m], whole, c_send.at[m, 0, 0], c_recv.at[m, 0, 0], {"dp": twin})

    for j in range(groups):
        taps[j, 0:n_taps, :] = cw_ref[:, j * LANES : (j + 1) * LANES].astype(jnp.float32)

    def forward_y(m, k, side, dd):
        start, size = gives(m)
        part = region(m, at_z(k), dd, start, size)
        send(part, part, y_send.at[m, k, side], y_recv.at[m, k, side], {"grp": 1 - y})

    def step_z(m, k):
        start, size = share(m)
        if k > 0:
            part = region(m, at_z(k), dp, start, size)
            remote(part, part, z_send.at[m, k - 1], z_recv.at[m, k - 1], {"sp": z}).wait_recv()
            send(part, part, x_send.at[m, k], x_recv.at[m, k], {"dp": across})
            forward_y(m, k, 0, dp)

    def step_x(m, k):
        start, size = share(m)
        part = region(m, at_z(k), across, start, size)
        remote(part, part, x_send.at[m, k], x_recv.at[m, k], {"dp": across}).wait_recv()
        forward_y(m, k, 1, across)

    def step_y(m, k):
        start, size = lacks(m)
        for side, dd in ((0, dp), (1, across)):
            if k == 0 and side == 0:
                continue
            part = region(m, at_z(k), dd, start, size)
            remote(part, part, y_send.at[m, k, side], y_recv.at[m, k, side], {"grp": 1 - y}).wait_recv()
            whole = region(m, at_z(k), dd, 0, own[m].shape[0])
            send(whole, whole, c_send.at[m, k, side], c_recv.at[m, k, side], {"dp": twin})

    def conv_group(j):
        tile = rows // 4
        for r in range(4):
            base = lead + r * tile
            total = jnp.zeros((tile, LANES), jnp.float32)
            for tap in range(n_taps):
                total = total + taps[j, tap : tap + 1, :] * ext[j, base - tap : base - tap + tile, :]
            conv[j, r * tile : (r + 1) * tile, :] = total.astype(jnp.bfloat16)

    def step_norm():
        tile = 2 * PACK
        channels = groups * LANES

        @pl.loop(0, rows // tile)
        def _(i):
            at = pl.ds(pl.multiple_of(i * tile, tile), tile)
            parts = [conv[j, at, :].astype(jnp.float32) for j in range(groups)]
            plain = functools.reduce(jnp.add, parts)
            square = functools.reduce(jnp.add, [p * p for p in parts])
            mean = jnp.sum(plain, axis=1, keepdims=True) * (1.0 / channels)
            meansq = jnp.sum(square, axis=1, keepdims=True) * (1.0 / channels)
            scale = lax.rsqrt(meansq - mean * mean + EPS)
            for j in range(groups):
                cols = slice(j * LANES, (j + 1) * LANES)
                v = (parts[j] - mean) * scale * gain_ref[:, cols] + bias_ref[:, cols]
                v = v / (1.0 + jnp.exp(-v))
                q, h = divmod(j, per_chunk)
                normed[q, at, h * LANES : (h + 1) * LANES] = v.astype(jnp.bfloat16)

    out_copies = []

    def step_use(m, k):
        zk = at_z(k)
        for side, dd in ((0, lax.rem(dp + 1 - 2 * core, n_dp)), (1, lax.rem(across + 1 - 2 * core, n_dp))):
            whole = region(m, zk, dd, 0, own[m].shape[0])
            remote(whole, whole, c_send.at[m, k, side], c_recv.at[m, k, side], {"dp": twin}).wait_recv()
        if k == 0:
            own_copies[m].wait()
            if m == 0:
                x_copy.wait()
                tail = xt.at[pl.ds(0, lead), :]
                remote(tail, tail, h_sem.at[0], h_sem.at[1], {"sp": z}).wait_recv()
        if m == 0:
            value[zk] = jnp.dot(xt[...], bv[zk], preferred_element_type=jnp.float32)
        elif m == 1:
            gate = jnp.dot(xt[...], bg[zk], preferred_element_type=jnp.float32)
            glu = (value[zk] * jax.nn.sigmoid(gate)).astype(jnp.bfloat16).astype(jnp.float32)
            before = jnp.where(z == 0, 0.0, 1.0)
            for h in range(per_chunk):
                cols = slice(h * LANES, (h + 1) * LANES)
                ext[zk * per_chunk + h, 0:lead, :] = glu[:lead, cols] * before
                ext[zk * per_chunk + h, lead:, :] = glu[lead:, cols]

            @pl.loop(0, per_chunk)
            def _(h):
                conv_group(zk * per_chunk + h)

            if k == n_sp - 1:
                step_norm()
        else:
            for d in range(n_dp):
                part = jnp.dot(normed[zk], bo[zk, d], preferred_element_type=jnp.float32)
                if k > 0:
                    part = part + acc[d]
                if k < n_sp - 1:
                    acc[d] = part
                else:
                    width = bo.shape[3]
                    stage[d] = part.astype(jnp.bfloat16)
                    copy = pltpu.make_async_copy(
                        stage.at[d], out_ref.at[:, d * width : (d + 1) * width], o_sem.at[d]
                    )
                    copy.start()
                    out_copies.append(copy)

    order = [(m, k) for m in range(3) for k in range(n_sp)]
    lags = ((step_z, 0), (step_x, 2), (step_y, 4), (step_use, 5))
    for t in range(len(order) + lags[-1][1]):
        for step, lag in lags:
            if 0 <= t - lag < len(order):
                step(*order[t - lag])

    for copy in started:
        copy.wait_send()
    for copy in out_copies:
        copy.wait()


def fused(n_sp, tokens, w_value, w_gate, conv_weight, norm_gain, norm_bias, w_out):
    rows, model = tokens.shape[1:]
    depth, chunk = w_value.shape
    deep, width = w_out.shape
    n_dp = model // depth
    n_taps, channels = conv_weight.shape
    lead = round_up(n_taps - 1, 2 * PACK)
    groups = channels // LANES
    total = rows + lead
    bf16, f32 = jnp.bfloat16, jnp.float32
    dma = pltpu.SemaphoreType.DMA
    anywhere = pl.BlockSpec(memory_space=pltpu.HBM)
    vmem = pl.BlockSpec(memory_space=pltpu.VMEM)
    out = pl.pallas_call(
        functools.partial(fused_kernel, n_sp),
        out_shape=jax.ShapeDtypeStruct((rows, model), bf16),
        in_specs=[anywhere] * 4 + [vmem] * 3,
        out_specs=anywhere,
        scratch_shapes=[
            pltpu.VMEM((n_sp, model, chunk), bf16),
            pltpu.VMEM((n_sp, model, chunk), bf16),
            pltpu.VMEM((n_sp, n_dp, deep, width), bf16),
            pltpu.VMEM((total, model), bf16),
            pltpu.VMEM((n_sp, total, chunk), f32),
            pltpu.VMEM((groups, total, LANES), f32),
            pltpu.VMEM((groups, round_up(n_taps, 8), LANES), f32),
            pltpu.VMEM((groups, rows, LANES), bf16),
            pltpu.VMEM((n_sp, rows, chunk), bf16),
            pltpu.VMEM((n_dp, rows, width), f32),
            pltpu.VMEM((n_dp, rows, width), bf16),
            dma((3, n_sp - 1)),
            dma((3, n_sp - 1)),
            dma((3, n_sp)),
            dma((3, n_sp)),
            dma((3, n_sp, 2)),
            dma((3, n_sp, 2)),
            dma((3, n_sp, 2)),
            dma((3, n_sp, 2)),
            dma((2,)),
            dma((4,)),
            dma((n_dp,)),
        ],
        compiler_params=pltpu.CompilerParams(
            collective_id=0, has_side_effects=True, vmem_limit_bytes=63 * 2**20
        ),
    )(tokens[0], w_value, w_gate, w_out, conv_weight, norm_gain[None], norm_bias[None])
    return out[None]


def passed_along(array, axis, by):
    peers = lax.axis_size(axis)
    pairs = [(i, i + by) for i in range(peers) if 0 <= i + by < peers]
    return lax.ppermute(array, axis, pairs)


def gathered(tokens, w_value, w_gate, conv_weight, norm_gain, norm_bias, w_out):
    pieces = (
        lax.all_gather(w_value, "sp", axis=1, tiled=True),
        lax.all_gather(w_gate, "sp", axis=1, tiled=True),
        lax.all_gather(w_out, "sp", axis=0, tiled=True),
    )
    full_value, full_gate, full_out = (
        lax.all_gather(pieces[0], "dp", axis=0, tiled=True),
        lax.all_gather(pieces[1], "dp", axis=0, tiled=True),
        lax.all_gather(pieces[2], "dp", axis=1, tiled=True),
    )
    rows = tokens[0]
    kernel_width = conv_weight.shape[0]
    channels = norm_gain.shape[0]
    value = jnp.dot(rows, full_value, preferred_element_type=jnp.float32)
    gate = jnp.dot(rows, full_gate, preferred_element_type=jnp.float32)
    glu = (value * jax.nn.sigmoid(gate)).astype(jnp.bfloat16)
    earlier = passed_along(glu[rows.shape[0] - (kernel_width - 1) :], "sp", 1)
    extended = jnp.concatenate([earlier, glu], axis=0)
    kernel = conv_weight[::-1][:, None, :]
    conv = lax.conv_general_dilated(
        extended[None],
        kernel,
        (1,),
        [(0, 0)],
        dimension_numbers=("NWC", "WIO", "NWC"),
        feature_group_count=channels,
        preferred_element_type=jnp.float32,
    )[0].astype(jnp.bfloat16)
    conv_f = conv.astype(jnp.float32)
    mean = jnp.mean(conv_f, axis=1, keepdims=True)
    meansq = jnp.mean(conv_f * conv_f, axis=1, keepdims=True)
    scaled = (conv_f - mean) * lax.rsqrt(meansq - mean * mean + EPS) * norm_gain + norm_bias
    normed = jax.nn.silu(scaled).astype(jnp.bfloat16)
    mixed = jnp.dot(normed, full_out, preferred_element_type=jnp.float32)
    return mixed.astype(jnp.bfloat16)[None]


def per_device(sizes, tokens, w_value, w_gate, conv_weight, norm_gain, norm_bias, w_out):
    args = (tokens, w_value, w_gate, conv_weight, norm_gain, norm_bias, w_out)
    pair_of_chips = sizes["grp"] == 2 and sizes["dp"] == 4
    whole_tiles = w_value.shape[1] % LANES == 0 and w_out.shape[1] % LANES == 0
    if pair_of_chips and whole_tiles and tokens.shape[0] == 1:
        return fused(sizes["sp"], *args)
    return gathered(*args)


def solution(mesh):
    placed = (
        P(("grp", "dp"), "sp", None),
        P("dp", "sp"),
        P("dp", "sp"),
        P(),
        P(),
        P(),
        P("sp", "dp"),
    )
    return jax.shard_map(
        functools.partial(per_device, dict(mesh.shape)),
        mesh=mesh,
        in_specs=placed,
        out_specs=P(("grp", "dp"), "sp", None),
        check_vma=False,
    )
```
